32 devices in a mesh: fs: 8 (over z, x), tp: 4 (over y, core).
Axes of the slice: x: 2, y: 2, z: 4, core: 2. Of those that a mesh axis runs over, the one named last changes fastest.
Arguments:
- h_saved: bfloat16 [16384, 2048], P('fs'), may hold values from -6 to 6
- conv_cotan: bfloat16 [16384, 2560], P('fs', 'tp'), may hold values from -64 to 64
- lru_out: bfloat16 [16384, 2560], P('fs', 'tp'), may hold values from -64 to 64
- out_cotan: bfloat16 [16384, 2048], P('fs'), may hold values from -6 to 6
- basis_in: bfloat16 [2048, 256], P('fs'), may hold values from -1.41421356 to 1.41421356
- basis_out: bfloat16 [2048, 256], P('fs'), may hold values from -1.41421356 to 1.41421356
- weight_in: float32 [2048, 2560], P('fs', 'tp'), may hold values from -0.125 to 0.125
- weight_out: float32 [2560, 2048], P('tp', 'fs'), may hold values from -0.125 to 0.125
- first_in: float32 [256, 2560], P('fs', 'tp'), may hold values from -6 to 6
- second_in: float32 [256, 2560], P('fs', 'tp'), may hold values from 0.05 to 2
- first_out: float32 [256, 2560], P('fs', 'tp'), may hold values from -6 to 6
- second_out: float32 [256, 2560], P('fs', 'tp'), may hold values from 0.05 to 2
Outputs:
- step_in: float32 [2048, 2560], P('fs', 'tp')
- new_weight_in: float32 [2048, 2560], P('fs', 'tp')
- copy_in: bfloat16 [2048, 2560], P(None, 'tp')
- new_first_in: float32 [256, 2560], P('fs', 'tp')
- new_second_in: float32 [256, 2560], P('fs', 'tp')
- step_out: float32 [2560, 2048], P('tp', 'fs')
- new_weight_out: float32 [2560, 2048], P('tp', 'fs')
- copy_out: bfloat16 [2560, 2048], P('tp')
- new_first_out: float32 [256, 2560], P('fs', 'tp')
- new_second_out: float32 [256, 2560], P('fs', 'tp')
The draws below stay inside these ranges and needn't reach their ends.
All inputs are finite; a program needn't handle non-finite values.
Results may differ from the reference program's by a relative error of at most 0.0046.
Values may be sent and summed in bfloat16 or wider, within the bound.
A program may use at most 128 MiB of HBM per device.

```python
import math
import jax
import jax.numpy as jnp
from jax import lax

D_MODEL = 2048
D_RNN = 2560
RANK = 256
TOKENS = 16384


def scaled_field(key, count, columns):
    keyone, keytwo = jax.random.split(key, 2)
    place = jnp.arange(columns, dtype=jnp.float32) / max(columns - 1, 1)
    rough = jnp.exp(jax.random.uniform(keytwo, (columns,), jnp.float32, math.log(0.5), math.log(2.0)))
    column_scale = jnp.exp(math.log(3.0) * place) * rough
    values = jnp.clip(jax.random.normal(keyone, (count, columns), jnp.float32), -6.0, 6.0)
    return values * column_scale


def draw_conv_cotan(key, part):
    return scaled_field(jax.random.fold_in(key, 11), TOKENS, D_RNN).astype(jnp.bfloat16)


def draw_lru_out(key, part):
    return scaled_field(jax.random.fold_in(key, 12), TOKENS, D_RNN).astype(jnp.bfloat16)


def draw_basis_in(key, part):
    return (scaled_field(jax.random.fold_in(key, 13), D_MODEL, RANK) / math.sqrt(D_MODEL)).astype(jnp.bfloat16)


def draw_basis_out(key, part):
    return (scaled_field(jax.random.fold_in(key, 14), D_MODEL, RANK) / math.sqrt(D_MODEL)).astype(jnp.bfloat16)


def block_scale(rng, dims, pieces, smallest, largest):
    level = 1.0
    for axis_at, blocks in pieces:
        steps = jax.random.uniform(jax.random.fold_in(jax.random.fold_in(rng, 6), axis_at), (blocks,), jnp.float32, smallest / len(pieces), largest / len(pieces))
        level = level * jnp.repeat(jnp.exp(steps), dims[axis_at] // blocks).reshape((-1,) + (1,) * (len(dims) - 1 - axis_at))
    return level


def scatter_about(stream_key, dims, width, most, shards=(), kind=jnp.bfloat16):
    loudness = block_scale(stream_key, dims, shards, -0.22, 0.18) if shards else 1.0
    values = jax.random.normal(stream_key, dims, jnp.float32) * width * loudness
    return jnp.minimum(jnp.maximum(values, -most), most).astype(kind)


def setup_inputs(seed: int = 0) -> dict:
    key_list = jax.random.split(jax.random.key(seed), 13)
    return {
        "h_saved": scatter_about(key_list[0], (TOKENS, D_MODEL), 1.0, 6.0, ((0, 8),)),
        "conv_cotan": draw_conv_cotan(jax.random.fold_in(key_list[12], 71), 0),
        "lru_out": draw_lru_out(jax.random.fold_in(key_list[12], 71), 0),
        "out_cotan": scatter_about(key_list[3], (TOKENS, D_MODEL), 1.0, 6.0, ((0, 8),)),
        "basis_in": draw_basis_in(jax.random.fold_in(key_list[12], 71), 0),
        "basis_out": draw_basis_out(jax.random.fold_in(key_list[12], 71), 0),
        "weight_in": scatter_about(key_list[6], (D_MODEL, D_RNN), D_MODEL ** -0.5, 0.125, ((0, 8), (1, 4)), jnp.float32),
        "weight_out": scatter_about(key_list[7], (D_RNN, D_MODEL), D_RNN ** -0.5, 0.125, ((0, 4), (1, 8)), jnp.float32),
        "first_in": scatter_about(key_list[8], (RANK, D_RNN), 1.0, 6.0, ((0, 8), (1, 4)), jnp.float32),
        "second_in": jnp.clip(jnp.exp(math.log(2.0) - 3.6888794 * jax.random.uniform(key_list[9], (RANK, D_RNN), jnp.float32) ** block_scale(key_list[9], (RANK, D_RNN), ((0, 8), (1, 4)), -0.2, 0.2)), 0.05, 2.0),
        "first_out": scatter_about(key_list[10], (RANK, D_RNN), 1.0, 6.0, ((0, 8), (1, 4)), jnp.float32),
        "second_out": jnp.clip(jnp.exp(math.log(2.0) - 3.6888794 * jax.random.uniform(key_list[11], (RANK, D_RNN), jnp.float32) ** block_scale(key_list[11], (RANK, D_RNN), ((0, 8), (1, 4)), -0.2, 0.2)), 0.05, 2.0),
    }


def exact_dot(left, right):
    return jnp.dot(left.astype(jnp.float32), right.astype(jnp.float32), precision=lax.Precision.HIGHEST)

def projected(inputs, cotan, basis):
    grad = exact_dot(inputs.T, cotan)
    return jnp.dot(basis.astype(jnp.float32).T, grad, precision=lax.Precision.HIGHEST)

def moments(proj, factor, first, second):
    scaled = factor * proj
    first_new = 0.8 * first + 0.2 * scaled
    second_new = 0.9 * second + 0.1 * scaled * scaled
    direction = (first_new / (jnp.sqrt(second_new) + 1e-08)).astype(jnp.bfloat16)
    return (first_new, second_new, direction)

def reference(h_saved, conv_cotan, lru_out, out_cotan, basis_in, basis_out, weight_in, weight_out, first_in, second_in, first_out, second_out):
    proj_in = projected(h_saved, conv_cotan, basis_in)
    proj_out = projected(out_cotan, lru_out, basis_out)
    total = jnp.sum(proj_in * proj_in) + jnp.sum(proj_out * proj_out)
    factor = math.sqrt(2.0 * RANK * D_RNN) * lax.rsqrt(total + 1e-06)
    first_a, second_a, dir_in = moments(proj_in, factor, first_in, second_in)
    first_b, second_b, dir_out = moments(proj_out, factor, first_out, second_out)
    step_in = exact_dot(basis_in, dir_in)
    step_out = exact_dot(basis_out, dir_out).T
    new_in = weight_in - 0.02 * step_in
    new_out = weight_out - 0.02 * step_out
    return (step_in, new_in, new_in.astype(jnp.bfloat16), first_a, second_a, step_out, new_out, new_out.astype(jnp.bfloat16), first_b, second_b)
```

```python
import functools
import math

import jax
import jax.numpy as jnp
from jax import lax
from jax.experimental import pallas as pl
from jax.experimental.pallas import tpu as pltpu
from jax.sharding import PartitionSpec as P

MESH = pl.DeviceIdType.MESH
VMEM_LIMIT = 42 * 1024 * 1024
FLUSH_LIMIT = 1024 * 1024
PIECES = 8
WINDOW = 3
AHEAD = 4


def nt_dot(left, right):
    return lax.dot_general(left, right, (((1,), (1,)), ((), ())), preferred_element_type=jnp.float32)


def exchange(
    dims,
    h_hbm,
    cc_hbm,
    oc_hbm,
    lo_hbm,
    basis_in,
    basis_out,
    w_in,
    w_out,
    m_in,
    v_in,
    m_out,
    v_out,
    step_in,
    new_in,
    copy_in,
    nm_in,
    nv_in,
    step_out,
    new_out,
    copy_out,
    nm_out,
    nv_out,
    ball,
    win_all,
    wout_all,
    dall,
    turned,
    h_buf,
    c_buf,
    acc,
    part,
    x_part,
    z_sum,
    z_part,
    tot,
    tot_in,
    in_sem,
    bx_s,
    bx_r,
    bz_s,
    bz_r,
    by_s,
    by_r,
    bm_s,
    bm_r,
    px_s,
    px_r,
    pz_s,
    pz_r,
    tot_s,
    tot_r,
    dx_s,
    dx_r,
    dz_s,
    dz_r,
    wd_s,
    wd_r,
    wu_s,
    wu_r,
    wx_s,
    wx_r,
):
    F, T, Z, X, scale = dims
    Y, Q = T // 2, PIECES
    f = lax.axis_index("fs")
    t = lax.axis_index("tp")
    z, x = f // X, f % X
    y, core = t // 2, t % 2
    mate = t + 1 - 2 * core
    turn = 1 - 2 * ((2 * z) // Z)
    chunks = in_sem.shape[1]
    chunk = h_buf.shape[1] // chunks
    rr, cols = m_in.shape
    rows, rank = basis_in.shape
    quarter = rows // T

    def remote(src, dst, send, recv, device):
        return pltpu.make_async_remote_copy(
            src_ref=src, dst_ref=dst, send_sem=send, recv_sem=recv, device_id=device, device_id_type=MESH
        )

    def z_peer(k):
        return ((z + k) % Z) * X + x

    def x_peer(j):
        return z * X + (x + j) % X

    def fetch(which, i):
        span = pl.ds(i * chunk, chunk)
        h_src, c_src = ((h_hbm, cc_hbm), (oc_hbm, lo_hbm))[which]
        return (
            pltpu.make_async_copy(h_src.at[span], h_buf.at[which, span], in_sem.at[which, i, 0]),
            pltpu.make_async_copy(c_src.at[span], c_buf.at[which, span], in_sem.at[which, i, 1]),
        )

    barrier = pltpu.get_barrier_semaphore()

    def greet(device):
        pl.semaphore_signal(barrier, inc=1, device_id=device, device_id_type=MESH)

    for k in range(1, Z):
        greet((z_peer(k), t))
    for j in range(1, X):
        greet((x_peer(j), t))
    for i in range(1, Y):
        greet((f, ((y + i) % Y) * 2 + core))
    greet((f, mate))
    for which in range(2):
        for i in range(chunks):
            for copy in fetch(which, i):
                copy.start()
    own = pl.ds(pl.multiple_of(t * quarter, quarter), quarter)
    for which, basis in enumerate((basis_in, basis_out)):
        ball[which, f] = basis[...]
    win_all[f] = w_in[...].astype(jnp.bfloat16)
    wout_all[f] = w_out[...].astype(jnp.bfloat16)
    pl.semaphore_wait(barrier, (Z - 1) + (X - 1) + (Y - 1) + 1)

    def row(m):
        return (z + turn * m + Z) % Z

    def basis_at(which, m, j, part_of):
        s = row(m) * X + (x + X - j) % X
        return ball.at[which, s, pl.ds(pl.multiple_of(part_of * quarter, quarter), quarter)]

    def basis_z(which, k):
        src = (basis_in, basis_out)[which].at[own]
        return remote(
            src, ball.at[which, f, own], bz_s.at[which, k], bz_r.at[which, z], (z_peer(k), t)
        )

    def basis_z_arrival(which, m):
        at = basis_at(which, m, 0, t)
        return remote(at, at, bz_s.at[which, m], bz_r.at[which, row(m)], (z_peer(1), t))

    def basis_x(which, m, j):
        at = basis_at(which, m, 0, t)
        src = at if m else (basis_in, basis_out)[which].at[own]
        return remote(src, at, bx_s.at[which, m, j], bx_r.at[which, m, j], (x_peer(j), t))

    def basis_x_arrival(which, m, j):
        at = basis_at(which, m, j, t)
        return remote(at, at, bx_s.at[which, m, j], bx_r.at[which, m, j], (x_peer(j), t))

    def basis_y(which, m, j, i, arrival=False):
        at = basis_at(which, m, j, ((y + Y - i) % Y) * 2 + core if arrival else t)
        return remote(
            at, at, by_s.at[which, m, j, i], by_r.at[which, m, j, i], (f, ((y + i) % Y) * 2 + core)
        )

    def basis_mate(which, m, j, i, arrival=False):
        at = basis_at(which, m, j, ((y + Y - i) % Y) * 2 + (1 - core if arrival else core))
        return remote(at, at, bm_s.at[which, m, j, i], bm_r.at[which, m, j, i], (f, mate))

    def basis_begin(which):
        for k in range(1, Z):
            basis_z(which, k).start()
        for j in range(1, X):
            basis_x(which, 0, j).start()

    def basis_spread(which, m, j):
        for i in range(1, Y):
            basis_y(which, m, j, i).start()
        basis_mate(which, m, j, 0).start()

    def basis_over_z(which):
        for m in range(1, Z):
            basis_z_arrival(which, m).wait_recv()
            for j in range(1, X):
                basis_x(which, m, j).start()
            basis_spread(which, m, 0)

    def basis_over_x(which):
        for m in range(Z):
            for j in range(1, X):
                basis_x_arrival(which, m, j).wait_recv()
                basis_spread(which, m, j)

    foreign = [(m, j) for j in range(X) for m in range(Z) if m or j]

    def basis_over_y(which):
        for m, j in foreign:
            for i in range(1, Y):
                basis_y(which, m, j, i, True).wait_recv()
                basis_mate(which, m, j, i).start()

    def basis_done(which):
        for m, j in foreign:
            for i in range(Y):
                basis_mate(which, m, j, i, True).wait_recv()

    in_rows, out_rows = w_in.shape[0] // Q, w_out.shape[0] // Q

    def place(item, s, q):
        if item == 0:
            return win_all.at[s, pl.ds(pl.multiple_of(q * in_rows, in_rows), in_rows)]
        return wout_all.at[s, pl.ds(pl.multiple_of(q * out_rows, out_rows), out_rows)]

    def down(m, q, item):
        at = place(item, (z + m) * X + x, q)
        return remote(at, at, wd_s.at[m, q, item], wd_r.at[m, q, item], ((z - 1) * X + x, t))

    def up(m, q, item):
        at = place(item, (z - m) * X + x, q)
        return remote(at, at, wu_s.at[m, q, item], wu_r.at[m, q, item], ((z + 1) * X + x, t))

    def aside(m, q, item, j):
        at = place(item, row(m) * X + x, q)
        return remote(at, at, wx_s.at[m, q, item, j], wx_r.at[m, q, item, j], (x_peer(j), t))

    def aside_arrival(m, q, item, j):
        at = place(item, row(m) * X + (x + X - j) % X, q)
        return remote(at, at, wx_s.at[m, q, item, j], wx_r.at[m, q, item, j], (x_peer(j), t))

    def down_arrival(m, q, item):
        at = place(item, (z + m) * X + x, q)
        return remote(at, at, wd_s.at[m - 1, q, item], wd_r.at[m - 1, q, item], (z_peer(1), t))

    def up_arrival(m, q, item):
        at = place(item, (z - m) * X + x, q)
        return remote(at, at, wu_s.at[m - 1, q, item], wu_r.at[m - 1, q, item], (z_peer(1), t))

    def goes_down(m):
        return (z >= 1) & (z + m <= Z - 1)

    def goes_up(m):
        return (z <= Z - 2) & (z - m >= 0)

    def z_settle(n):
        m, q = n // Q, n % Q

        @pl.when((n >= 0) & goes_down(m))
        def _():
            for item in range(2):
                down(m, q, item).wait_send()

        @pl.when((n >= 0) & goes_up(m))
        def _():
            for item in range(2):
                up(m, q, item).wait_send()

    def z_arrivals(n):
        m, q = n // Q, n % Q

        @pl.when((m >= 1) & (m <= Z - 1) & (z + m <= Z - 1))
        def _():
            for item in range(2):
                down_arrival(m, q, item).wait_recv()

        @pl.when((m >= 1) & (m <= Z - 1) & (z - m >= 0))
        def _():
            for item in range(2):
                up_arrival(m, q, item).wait_recv()

    def z_tick(n):
        m, q = n // Q, n % Q
        z_arrivals(n + AHEAD)
        z_settle(n - WINDOW)

        @pl.when(goes_down(m))
        def _():
            for item in range(2):
                down(m, q, item).start()

        @pl.when(goes_up(m))
        def _():
            for item in range(2):
                up(m, q, item).start()

    def x_settle(n):
        @pl.when(n >= 0)
        def _():
            for item in range(2):
                for j in range(1, X):
                    aside(n // Q, n % Q, item, j).wait_send()

    def x_tick(n):
        x_settle(n - WINDOW)
        for item in range(2):
            for j in range(1, X):
                aside(n // Q, n % Q, item, j).start()

    ticks = Z * Q
    passed = [0, 0]

    def loop(low, high, body):
        def step(n, carry):
            body(n)
            return carry

        if high > low:
            lax.fori_loop(low, high, step, 0)

    def pump(z_count, x_count):
        z_at, x_at = passed
        z_count, x_count = max(0, min(z_count, ticks - z_at)), max(0, min(x_count, ticks - x_at))
        both = min(z_count, x_count)

        def pair(n):
            z_tick(z_at + n)
            x_tick(x_at + n)

        loop(0, both, pair)
        loop(z_at + both, z_at + z_count, z_tick)
        loop(x_at + both, x_at + x_count, x_tick)
        passed[0], passed[1] = z_at + z_count, x_at + x_count
        assert passed[1] <= max(Q, passed[0] + AHEAD)

    def project(which, during):
        acc[which] = jnp.zeros(acc.shape[1:], jnp.float32)
        for i in range(chunks):
            for copy in fetch(which, i):
                copy.wait()
            span = pl.ds(i * chunk, chunk)
            whole = ball[which].reshape(h_buf.shape[2], -1)
            reduced = jnp.dot(h_buf[which, span], whole, preferred_element_type=jnp.float32)
            turned = reduced.T
            upper = turned.astype(jnp.bfloat16)
            lower = (turned - upper.astype(jnp.float32)).astype(jnp.bfloat16)
            block = c_buf[which, span]
            acc[which] += jnp.dot(upper, block, preferred_element_type=jnp.float32) + jnp.dot(
                lower, block, preferred_element_type=jnp.float32
            )
            during(i)
        part[which] = acc[which].astype(jnp.bfloat16).reshape(part.shape[1:])

    def part_x(which, j):
        return remote(
            part.at[which, pl.ds(0, Z), (x + j) % X],
            x_part.at[which, j],
            px_s.at[which, j],
            px_r.at[which, j],
            (x_peer(j), t),
        )

    def part_z(which, k):
        return remote(
            z_sum.at[which, (z + k) % Z],
            z_part.at[which, k],
            pz_s.at[which, k],
            pz_r.at[which, k],
            (z_peer(k), t),
        )

    def row_sum(which, to):
        value = acc[which, pl.ds(pl.multiple_of((to * X + x) * rr, rr), rr)]
        for j in range(1, X):
            value = value + x_part[which, j, to].astype(jnp.float32)
        return value

    def reduce_x(which):
        for j in range(1, X):
            part_x(which, j).wait_recv()
        for to in range(Z):
            z_sum[which, to] = row_sum(which, to).astype(jnp.bfloat16)
        for k in range(1, Z):
            part_z(which, k).start()

    def reduce_z(which):
        value = row_sum(which, z)
        for k in range(1, Z):
            part_z(which, k).wait_recv()
            value = value + z_part[which, k].astype(jnp.float32)
        return value

    def share(n):
        return remote(
            tot,
            tot_in.at[n],
            tot_s.at[n],
            tot_r.at[n],
            ((f + n // T) % F, (t + n % T) % T),
        )

    def dir_z(k):
        return remote(dall.at[f], dall.at[f], dz_s.at[k], dz_r.at[z], (z_peer(k), t))

    def dir_z_arrival(m):
        at = dall.at[row(m) * X + x]
        return remote(at, at, dz_s.at[m], dz_r.at[row(m)], (z_peer(1), t))

    def dir_x(m, j, arrival=False):
        at = dall.at[row(m) * X + ((x + X - j) % X if arrival else x)]
        return remote(at, at, dx_s.at[m, j], dx_r.at[m, j], (x_peer(j), t))

    def late(m):
        def each(q):
            for item in range(2):
                for j in range(1, X):
                    aside_arrival(m, q, item, j).wait_recv()

        loop(0, Q, each)

    def apply_own():
        direction = dall[:, 0].reshape(rank, cols)
        other = dall[:, 1].reshape(rank, cols)
        turned[...] = other.astype(jnp.float32).T.astype(jnp.bfloat16)
        step = jnp.dot(basis_in[...], direction, preferred_element_type=jnp.float32)
        step_in[...] = step
        new_in[...] = w_in[...] - 0.02 * step
        step = nt_dot(turned[...], basis_out[...])
        step_out[...] = step
        new_out[...] = w_out[...] - 0.02 * step

    def apply_row(m):
        direction = dall[:, 0].reshape(rank, cols)
        for j in range(X):
            s = row(m) * X + j
            span = pl.ds(pl.multiple_of(s * rows, rows), rows)
            step = jnp.dot(ball[0, s], direction, preferred_element_type=jnp.float32)
            copy_in[span] = (win_all[s].astype(jnp.float32) - 0.02 * step).astype(jnp.bfloat16)
            step = nt_dot(turned[...], ball[1, s])
            copy_out[:, span] = (wout_all[s].astype(jnp.float32) - 0.02 * step).astype(jnp.bfloat16)

    for which in range(2):
        basis_begin(which)
    pump(1, 1)
    basis_over_z(0)
    basis_over_z(1)
    pump(1, 1)
    basis_over_x(0)
    basis_over_x(1)
    pump(1, 1)
    basis_over_y(0)
    basis_done(0)

    def meanwhile(i):
        pump(1, 1)

    project(0, meanwhile)
    for j in range(1, X):
        part_x(0, j).start()
    basis_over_y(1)
    basis_done(1)

    def meanwhile(i):
        if i == 2:
            reduce_x(0)
        pump(1, 1)

    project(1, meanwhile)
    for j in range(1, X):
        part_x(1, j).start()
    pump(1, 1)
    reduce_x(1)
    pump(2, 2)
    projs = [reduce_z(which) for which in range(2)]
    square = sum(jnp.sum(value * value, axis=(0, 1), keepdims=True) for value in projs)
    tot[...] = jnp.broadcast_to(square, tot.shape)
    tot_in[0] = tot[...]
    loop(1, F * T, lambda n: share(n).start())
    pump(1, 1)
    loop(1, F * T, lambda n: share(n).wait())
    total = jnp.sum(jnp.sum(tot_in[...], axis=0), axis=0, keepdims=True)
    factor = (scale * lax.rsqrt(total + 1e-06))[0:1, 0:1]
    for which, (first, second, first_to, second_to) in enumerate(
        ((m_in, v_in, nm_in, nv_in), (m_out, v_out, nm_out, nv_out))
    ):
        scaled = factor * projs[which]
        first_new = 0.8 * first[...] + 0.2 * scaled
        second_new = 0.9 * second[...] + 0.1 * scaled * scaled
        first_to[...] = first_new
        second_to[...] = second_new
        dall[f, which] = (first_new / (jnp.sqrt(second_new) + 1e-08)).astype(jnp.bfloat16)
    for k in range(1, Z):
        dir_z(k).start()
    for j in range(1, X):
        dir_x(0, j).start()
    pump(2, 2)
    for m in range(1, Z):
        dir_z_arrival(m).wait_recv()
        for j in range(1, X):
            dir_x(m, j).start()
    pump(2, 2)
    for m in range(Z):
        for j in range(1, X):
            dir_x(m, j, True).wait_recv()
    apply_own()
    for m in range(Z):
        pump((m + 1) * Q - passed[1], (m + 1) * Q - passed[1])
        late(m)
        apply_row(m)
    pump(ticks, ticks)

    loop(ticks - WINDOW, ticks, z_settle)
    loop(ticks - WINDOW, ticks, x_settle)
    for which in range(2):
        for k in range(1, Z):
            basis_z(which, k).wait_send()
            part_z(which, k).wait_send()
        for j in range(1, X):
            part_x(which, j).wait_send()
            for m in range(Z):
                basis_x(which, m, j).wait_send()
        for m, j in foreign:
            for i in range(Y):
                if i:
                    basis_y(which, m, j, i).wait_send()
                basis_mate(which, m, j, i).wait_send()
    for k in range(1, Z):
        dir_z(k).wait_send()
    for m in range(Z):
        for j in range(1, X):
            dir_x(m, j).wait_send()


def flush(*refs):
    sources, targets, sems = refs[:10], refs[10:20], refs[20]
    copies = [pltpu.make_async_copy(a, b, sems.at[i]) for i, (a, b) in enumerate(zip(sources, targets))]
    for copy in copies:
        copy.start()
    for copy in copies:
        copy.wait()


def shards(mesh, h, cc, lo, oc, basis_in, basis_out, w_in, w_out, m_in, v_in, m_out, v_out):
    F, T = mesh.shape["fs"], mesh.shape["tp"]
    Z = next(n for n in range(1, F + 1) if F % n == 0 and n * n >= F)
    X, Y = F // Z, T // 2
    tokens, model = h.shape
    cols = cc.shape[1]
    rows, rank = basis_in.shape
    rr = m_in.shape[0]
    scale = math.sqrt(2.0 * rank * cols * T)
    chunks = max(1, tokens // 512)
    bf, f32 = jnp.bfloat16, jnp.float32
    hbm = pl.BlockSpec(memory_space=pl.ANY)
    vmem = pl.BlockSpec(memory_space=pltpu.VMEM)
    local = (w_in.shape, w_in.shape, (model, cols), m_in.shape, m_in.shape)
    local += (w_out.shape, w_out.shape, (cols, model), m_in.shape, m_in.shape)
    outs = tuple(jax.ShapeDtypeStruct(shape, bf if n in (2, 7) else f32) for n, shape in enumerate(local))

    def dma(*shape):
        return [pltpu.SemaphoreType.DMA(shape)] * 2

    results = pl.pallas_call(
        functools.partial(exchange, (F, T, Z, X, scale)),
        out_shape=outs,
        in_specs=[hbm] * 4 + [vmem] * 8,
        out_specs=(vmem,) * 10,
        scratch_shapes=[
            pltpu.VMEM((2, F, rows, rank), bf),
            pltpu.VMEM((F,) + w_in.shape, bf),
            pltpu.VMEM((F,) + w_out.shape, bf),
            pltpu.VMEM((F, 2, rr, cols), bf),
            pltpu.VMEM((cols, rank), bf),
            pltpu.VMEM((2, tokens, model), bf),
            pltpu.VMEM((2, tokens, cols), bf),
            pltpu.VMEM((2, rank, cols), f32),
            pltpu.VMEM((2, Z, X, rr, cols), bf),
            pltpu.VMEM((2, X, Z, rr, cols), bf),
            pltpu.VMEM((2, Z, rr, cols), bf),
            pltpu.VMEM((2, Z, rr, cols), bf),
            pltpu.VMEM((1, 128), f32),
            pltpu.VMEM((F * T, 1, 128), f32),
            pltpu.SemaphoreType.DMA((2, chunks, 2)),
            *dma(2, Z, X),
            *dma(2, Z),
            *dma(2, Z, X, Y),
            *dma(2, Z, X, Y),
            *dma(2, X),
            *dma(2, Z),
            *dma(F * T),
            *dma(Z, X),
            *dma(Z),
            *dma(Z, PIECES, 2),
            *dma(Z, PIECES, 2),
            *dma(Z, PIECES, 2, X),
        ],
        compiler_params=pltpu.CompilerParams(
            collective_id=0, has_side_effects=True, vmem_limit_bytes=VMEM_LIMIT
        ),
        name="exchange",
    )(h, cc, oc, lo, basis_in, basis_out, w_in, w_out, m_in, v_in, m_out, v_out)

    return pl.pallas_call(
        flush,
        out_shape=outs,
        in_specs=[hbm] * 10,
        out_specs=(hbm,) * 10,
        scratch_shapes=[pltpu.SemaphoreType.DMA((10,))],
        compiler_params=pltpu.CompilerParams(vmem_limit_bytes=FLUSH_LIMIT),
        name="flush",
    )(*results)


def solution(mesh):
    split, both = P("fs", None), P("fs", "tp")
    return jax.shard_map(
        functools.partial(shards, mesh),
        mesh=mesh,
        in_specs=(split, both, both, split, split, split, both, P("tp", "fs"), both, both, both, both),
        out_specs=(both, both, P(None, "tp"), both, both, P("tp", "fs"), P("tp", "fs"), P("tp", None), both, both),
        check_vma=False,
    )
```

```python
import functools
import math

import jax
import jax.numpy as jnp
from jax import lax
from jax.experimental import pallas as pl
from jax.experimental.pallas import tpu as pltpu
from jax.sharding import PartitionSpec as P

MESH = pl.DeviceIdType.MESH
VMEM_LIMIT = 42 * 1024 * 1024
FLUSH_LIMIT = 1024 * 1024
PIECES = 8
WINDOW = 3
AHEAD = 4
PLAN = [(3, 3), (3, 3), (2, 2), [(1, 1), (1, 1), (1, 1), (1, 1)], [(1, 1), (1, 1), (1, 1), (1, 1)], (2, 2), (3, 3), (2, 2), (3, 3), (3, 3)]


def nt_dot(left, right):
    return lax.dot_general(left, right, (((1,), (1,)), ((), ())), preferred_element_type=jnp.float32)


def exchange(
    dims,
    h_hbm,
    cc_hbm,
    oc_hbm,
    lo_hbm,
    basis_in,
    basis_out,
    w_in_hbm,
    w_out_hbm,
    m_in_hbm,
    v_in_hbm,
    m_out_hbm,
    v_out_hbm,
    step_in,
    new_in,
    copy_in,
    nm_in,
    nv_in,
    step_out,
    new_out,
    copy_out,
    nm_out,
    nv_out,
    ball,
    win_all,
    wout_all,
    dall,
    turned,
    h_buf,
    c_buf,
    acc,
    part,
    x_part,
    z_sum,
    z_part,
    tot,
    tot_in,
    w_in,
    w_out,
    m_in,
    v_in,
    m_out,
    v_out,
    in_sem,
    load_sem,
    b_s,
    bz_r,
    bx_r,
    by_r,
    bm_r,
    p_s,
    px_r,
    pz_r,
    tot_sem,
    d_s,
    dz_r,
    dx_r,
    w_s,
    wd_r,
    wu_r,
    wx_r,
):
    F, T, Z, X, scale = dims
    Y, Q = T // 2, PIECES
    f = lax.axis_index("fs")
    t = lax.axis_index("tp")
    z, x = f // X, f % X
    y, core = t // 2, t % 2
    mate = t + 1 - 2 * core
    turn = 1 - 2 * ((2 * z) // Z)
    chunks = in_sem.shape[1]
    chunk = h_buf.shape[1] // chunks
    rr, cols = m_in.shape
    rows, rank = ball.shape[2:]
    quarter = rows // T

    def remote(src, dst, send, recv, device):
        return pltpu.make_async_remote_copy(
            src_ref=src, dst_ref=dst, send_sem=send, recv_sem=recv, device_id=device, device_id_type=MESH
        )

    def settle(ref, sem):
        pltpu.make_async_copy(ref, ref, sem).wait()

    def z_peer(k):
        return ((z + k) % Z) * X + x

    def x_peer(j):
        return z * X + (x + j) % X

    def fetch(which, i):
        span = pl.ds(i * chunk, chunk)
        h_src, c_src = ((h_hbm, cc_hbm), (oc_hbm, lo_hbm))[which]
        return (
            pltpu.make_async_copy(h_src.at[span], h_buf.at[which, span], in_sem.at[which, i, 0]),
            pltpu.make_async_copy(c_src.at[span], c_buf.at[which, span], in_sem.at[which, i, 1]),
        )

    barrier = pltpu.get_barrier_semaphore()

    def greet(device):
        pl.semaphore_signal(barrier, inc=1, device_id=device, device_id_type=MESH)

    for k in range(1, Z):
        greet((z_peer(k), t))
    for j in range(1, X):
        greet((x_peer(j), t))
    for i in range(1, Y):
        greet((f, ((y + i) % Y) * 2 + core))
    greet((f, mate))
    loads = [
        pltpu.make_async_copy(src, dst, load_sem.at[n])
        for n, (src, dst) in enumerate(
            (
                (basis_in, ball.at[0, f]),
                (basis_out, ball.at[1, f]),
                (w_in_hbm, w_in),
                (w_out_hbm, w_out),
                (m_in_hbm, m_in),
                (v_in_hbm, v_in),
                (m_out_hbm, m_out),
                (v_out_hbm, v_out),
            )
        )
    ]
    for copy in loads:
        copy.start()
    for which in range(2):
        for i in range(chunks):
            for copy in fetch(which, i):
                copy.start()
    own = pl.ds(pl.multiple_of(t * quarter, quarter), quarter)
    for copy in loads:
        copy.wait()
    win_all[f] = w_in[...].astype(jnp.bfloat16)
    wout_all[f] = w_out[...].astype(jnp.bfloat16)
    pl.semaphore_wait(barrier, (Z - 1) + (X - 1) + (Y - 1) + 1)

    def row(m):
        return (z + turn * m + Z) % Z

    def basis_at(which, m, j, part_of):
        s = row(m) * X + (x + X - j) % X
        return ball.at[which, s, pl.ds(pl.multiple_of(part_of * quarter, quarter), quarter)]

    def basis_z(which, k):
        at = ball.at[which, f, own]
        return remote(at, at, b_s.at[0], bz_r.at[which, z], (z_peer(k), t))

    def basis_z_arrival(which, m):
        at = basis_at(which, m, 0, t)
        return remote(at, at, b_s.at[0], bz_r.at[which, row(m)], (z_peer(1), t))

    def basis_x(which, m, j):
        at = basis_at(which, m, 0, t)
        return remote(at, at, b_s.at[1], bx_r.at[which, m, j - 1], (x_peer(j), t))

    def basis_x_arrival(which, m, j):
        at = basis_at(which, m, j, t)
        return remote(at, at, b_s.at[1], bx_r.at[which, m, j - 1], (x_peer(j), t))

    def basis_y(which, m, j, i):
        at = basis_at(which, m, j, t)
        return remote(at, at, b_s.at[2], by_r.at[which], (f, ((y + i) % Y) * 2 + core))

    def basis_mate(which, m, j, i):
        at = basis_at(which, m, j, ((y + Y - i) % Y) * 2 + core)
        return remote(at, at, b_s.at[3], bm_r.at[which], (f, mate))

    def basis_begin(which):
        for k in range(1, Z):
            basis_z(which, k).start()
        for j in range(1, X):
            basis_x(which, 0, j).start()

    def basis_spread(which, m, j):
        for i in range(1, Y):
            basis_y(which, m, j, i).start()
        basis_mate(which, m, j, 0).start()

    def basis_over_z(which):
        for m in range(1, Z):
            basis_z_arrival(which, m).wait_recv()
            for j in range(1, X):
                basis_x(which, m, j).start()
            basis_spread(which, m, 0)

    def basis_over_x(which):
        for m in range(Z):
            for j in range(1, X):
                basis_x_arrival(which, m, j).wait_recv()
                basis_spread(which, m, j)

    foreign = [(m, j) for j in range(X) for m in range(Z) if m or j]

    def basis_bytes(whiches, shares):
        return ball.at[whiches, pl.ds(0, F - 1), pl.ds(0, shares * quarter)]

    def basis_over_y(which):
        if Y > 1:
            settle(basis_bytes(which, Y - 1), by_r.at[which])
        for m, j in foreign:
            for i in range(1, Y):
                basis_mate(which, m, j, i).start()

    def basis_done(which):
        settle(basis_bytes(which, Y), bm_r.at[which])

    in_rows, out_rows = 2 * w_in.shape[0] // Q, 2 * w_out.shape[0] // Q

    def place(item, s, q):
        if item == 0:
            return win_all.at[s, pl.ds(pl.multiple_of((q // 2) * in_rows, in_rows), in_rows)]
        return wout_all.at[s, pl.ds(pl.multiple_of((q // 2) * out_rows, out_rows), out_rows)]

    def turns(q, body):
        for item in range(2):

            @pl.when(q % 2 == item)
            def _(item=item):
                body(item)

    def down(n, item):
        m, q = n // Q, n % Q
        at = place(item, (z + m) * X + x, q)
        return remote(at, at, w_s.at[0, n % WINDOW, 0], wd_r.at[m, q], ((z - 1) * X + x, t))

    def up(n, item):
        m, q = n // Q, n % Q
        at = place(item, (z - m) * X + x, q)
        return remote(at, at, w_s.at[1, n % WINDOW, 0], wu_r.at[m, q], ((z + 1) * X + x, t))

    def aside(n, item, j):
        m, q = n // Q, n % Q
        at = place(item, row(m) * X + x, q)
        return remote(
            at, at, w_s.at[2, n % WINDOW, j - 1], wx_r.at[m, q, j - 1], (x_peer(j), t)
        )

    def aside_arrival(n, item, j):
        m, q = n // Q, n % Q
        at = place(item, row(m) * X + (x + X - j) % X, q)
        return remote(at, at, w_s.at[2, 0, j - 1], wx_r.at[m, q, j - 1], (x_peer(j), t))

    def down_arrival(n, item):
        m, q = n // Q, n % Q
        at = place(item, (z + m) * X + x, q)
        return remote(at, at, w_s.at[0, 0, 0], wd_r.at[m - 1, q], (z_peer(1), t))

    def up_arrival(n, item):
        m, q = n // Q, n % Q
        at = place(item, (z - m) * X + x, q)
        return remote(at, at, w_s.at[1, 0, 0], wu_r.at[m - 1, q], (z_peer(1), t))

    def goes_down(m):
        return (z >= 1) & (z + m <= Z - 1)

    def goes_up(m):
        return (z <= Z - 2) & (z - m >= 0)

    def z_settle(n):
        m, q = n // Q, n % Q

        @pl.when((n >= 0) & goes_down(m))
        def _():
            turns(q, lambda item: down(n, item).wait_send())

        @pl.when((n >= 0) & goes_up(m))
        def _():
            turns(q, lambda item: up(n, item).wait_send())

    def z_arrivals(n):
        m, q = n // Q, n % Q

        @pl.when((m >= 1) & (m <= Z - 1) & (z + m <= Z - 1))
        def _():
            turns(q, lambda item: down_arrival(n, item).wait_recv())

        @pl.when((m >= 1) & (m <= Z - 1) & (z - m >= 0))
        def _():
            turns(q, lambda item: up_arrival(n, item).wait_recv())

    def z_tick(n):
        m, q = n // Q, n % Q
        z_arrivals(n + AHEAD)
        z_settle(n - WINDOW)

        @pl.when(goes_down(m))
        def _():
            turns(q, lambda item: down(n, item).start())

        @pl.when(goes_up(m))
        def _():
            turns(q, lambda item: up(n, item).start())

    def x_settle(n):
        @pl.when(n >= 0)
        def _():
            for j in range(1, X):
                turns(n % Q, lambda item: aside(n, item, j).wait_send())

    def x_tick(n):
        x_settle(n - WINDOW)
        for j in range(1, X):
            turns(n % Q, lambda item: aside(n, item, j).start())

    ticks = Z * Q
    passed = [0, 0]

    def loop(low, high, body):
        def step(n, carry):
            body(n)
            return carry

        if high > low:
            lax.fori_loop(low, high, step, 0)

    def pump(z_count, x_count):
        z_at, x_at = passed
        z_count, x_count = max(0, min(z_count, ticks - z_at)), max(0, min(x_count, ticks - x_at))
        both = min(z_count, x_count)

        def pair(n):
            z_tick(z_at + n)
            x_tick(x_at + n)

        loop(0, both, pair)
        loop(z_at + both, z_at + z_count, z_tick)
        loop(x_at + both, x_at + x_count, x_tick)
        passed[0], passed[1] = z_at + z_count, x_at + x_count
        assert passed[1] <= max(Q, passed[0] + AHEAD)

    def project(which, during):
        acc[which] = jnp.zeros(acc.shape[1:], jnp.float32)
        for i in range(chunks):
            for copy in fetch(which, i):
                copy.wait()
            span = pl.ds(i * chunk, chunk)
            whole = ball[which].reshape(h_buf.shape[2], -1)
            reduced = jnp.dot(h_buf[which, span], whole, preferred_element_type=jnp.float32)
            turned_bf = reduced.T.astype(jnp.bfloat16)
            acc[which] += jnp.dot(turned_bf, c_buf[which, span], preferred_element_type=jnp.float32)
            during(i)
        part[which] = acc[which].astype(jnp.bfloat16).reshape(part.shape[1:])

    def part_x(which, j):
        return remote(
            part.at[which, pl.ds(0, Z), (x + j) % X],
            x_part.at[which, j],
            p_s.at[0],
            px_r.at[which, j - 1],
            (x_peer(j), t),
        )

    def part_z(which, k):
        return remote(
            z_sum.at[which, (z + k) % Z], z_part.at[which, k], p_s.at[1], pz_r.at[which], (z_peer(k), t)
        )

    def row_sum(which, to):
        value = acc[which, pl.ds(pl.multiple_of((to * X + x) * rr, rr), rr)]
        for j in range(1, X):
            value = value + x_part[which, j, to].astype(jnp.float32)
        return value

    def reduce_x(which):
        for j in range(1, X):
            part_x(which, j).wait_recv()
        for to in range(Z):
            z_sum[which, to] = row_sum(which, to).astype(jnp.bfloat16)
        for k in range(1, Z):
            part_z(which, k).start()

    def reduce_z(which):
        value = row_sum(which, z)
        settle(z_part.at[which, pl.ds(1, Z - 1)], pz_r.at[which])
        for k in range(1, Z):
            value = value + z_part[which, k].astype(jnp.float32)
        return value

    def share(n):
        return remote(
            tot,
            tot_in.at[n],
            tot_sem.at[0],
            tot_sem.at[1],
            ((f + n // T) % F, (t + n % T) % T),
        )

    def dir_z(k):
        return remote(dall.at[f], dall.at[f], d_s.at[0], dz_r.at[z], (z_peer(k), t))

    def dir_z_arrival(m):
        at = dall.at[row(m) * X + x]
        return remote(at, at, d_s.at[0], dz_r.at[row(m)], (z_peer(1), t))

    def dir_x(m, j):
        at = dall.at[row(m) * X + x]
        return remote(at, at, d_s.at[1], dx_r.at[0], (x_peer(j), t))

    def late(m):
        def each(q):
            for j in range(1, X):
                turns(q, lambda item: aside_arrival(m * Q + q, item, j).wait_recv())

        loop(0, Q, each)

    def apply_own():
        direction = dall[:, 0].reshape(rank, cols)
        other = dall[:, 1].reshape(rank, cols)
        turned[...] = other.astype(jnp.float32).T.astype(jnp.bfloat16)
        step = jnp.dot(ball[0, f], direction, preferred_element_type=jnp.float32)
        step_in[...] = step
        new_in[...] = w_in[...] - 0.02 * step
        step = nt_dot(turned[...], ball[1, f])
        step_out[...] = step
        new_out[...] = w_out[...] - 0.02 * step

    def apply_row(m):
        direction = dall[:, 0].reshape(rank, cols)
        for j in range(X):
            s = row(m) * X + j
            span = pl.ds(pl.multiple_of(s * rows, rows), rows)
            step = jnp.dot(ball[0, s], direction, preferred_element_type=jnp.float32)
            copy_in[span] = (win_all[s].astype(jnp.float32) - 0.02 * step).astype(jnp.bfloat16)
            step = nt_dot(turned[...], ball[1, s])
            copy_out[:, span] = (wout_all[s].astype(jnp.float32) - 0.02 * step).astype(jnp.bfloat16)

    for which in range(2):
        basis_begin(which)
    pump(*PLAN[0])
    basis_over_z(0)
    basis_over_z(1)
    pump(*PLAN[1])
    basis_over_x(0)
    basis_over_x(1)
    pump(*PLAN[2])
    basis_over_y(0)
    basis_done(0)
    project(0, lambda i: pump(*PLAN[3][i]))
    for j in range(1, X):
        part_x(0, j).start()
    basis_over_y(1)
    basis_done(1)

    def meanwhile(i):
        if i == 2:
            reduce_x(0)
        pump(*PLAN[4][i])

    project(1, meanwhile)
    for j in range(1, X):
        part_x(1, j).start()
    pump(*PLAN[5])
    reduce_x(1)
    pump(*PLAN[6])
    projs = [reduce_z(which) for which in range(2)]
    square = sum(jnp.sum(value * value, axis=(0, 1), keepdims=True) for value in projs)
    tot[...] = jnp.broadcast_to(square, tot.shape)
    tot_in[0] = tot[...]
    loop(1, F * T, lambda n: share(n).start())
    pump(*PLAN[7])
    for sem in range(2):
        settle(tot_in.at[pl.ds(1, F * T - 1)], tot_sem.at[sem])
    total = jnp.sum(jnp.sum(tot_in[...], axis=0), axis=0, keepdims=True)
    factor = (scale * lax.rsqrt(total + 1e-06))[0:1, 0:1]
    for which, (first, second, first_to, second_to) in enumerate(
        ((m_in, v_in, nm_in, nv_in), (m_out, v_out, nm_out, nv_out))
    ):
        scaled = factor * projs[which]
        first_new = 0.8 * first[...] + 0.2 * scaled
        second_new = 0.9 * second[...] + 0.1 * scaled * scaled
        first_to[...] = first_new
        second_to[...] = second_new
        dall[f, which] = (first_new / (jnp.sqrt(second_new) + 1e-08)).astype(jnp.bfloat16)
    for k in range(1, Z):
        dir_z(k).start()
    for j in range(1, X):
        dir_x(0, j).start()
    pump(*PLAN[8])
    for m in range(1, Z):
        dir_z_arrival(m).wait_recv()
        for j in range(1, X):
            dir_x(m, j).start()
    pump(*PLAN[9])
    settle(dall.at[pl.ds(0, Z * (X - 1))], dx_r.at[0])
    apply_own()
    for m in range(Z):
        pump((m + 1) * Q - passed[1], (m + 1) * Q - passed[1])
        late(m)
        apply_row(m)
    pump(ticks, ticks)

    loop(ticks - WINDOW, ticks, z_settle)
    loop(ticks - WINDOW, ticks, x_settle)
    both = pl.ds(0, 2)
    settle(ball.at[both, pl.ds(0, Z - 1), pl.ds(0, quarter)], b_s.at[0])
    settle(ball.at[both, pl.ds(0, Z * (X - 1)), pl.ds(0, quarter)], b_s.at[1])
    if Y > 1:
        settle(basis_bytes(both, Y - 1), b_s.at[2])
    settle(basis_bytes(both, Y), b_s.at[3])
    settle(part.at[both, pl.ds(0, Z), pl.ds(0, X - 1)], p_s.at[0])
    settle(z_sum.at[both, pl.ds(0, Z - 1)], p_s.at[1])
    settle(dall.at[pl.ds(0, Z - 1)], d_s.at[0])
    settle(dall.at[pl.ds(0, Z * (X - 1))], d_s.at[1])


def flush(*refs):
    sources, targets, sems = refs[:10], refs[10:20], refs[20]
    copies = [pltpu.make_async_copy(a, b, sems.at[i]) for i, (a, b) in enumerate(zip(sources, targets))]
    for copy in copies:
        copy.start()
    for copy in copies:
        copy.wait()


def shards(mesh, h, cc, lo, oc, basis_in, basis_out, w_in, w_out, m_in, v_in, m_out, v_out):
    F, T = mesh.shape["fs"], mesh.shape["tp"]
    Z = next(n for n in range(1, F + 1) if F % n == 0 and n * n >= F)
    X, Y = F // Z, T // 2
    tokens, model = h.shape
    cols = cc.shape[1]
    rows, rank = basis_in.shape
    rr = m_in.shape[0]
    scale = math.sqrt(2.0 * rank * cols * T)
    chunks = max(1, tokens // 512)
    bf, f32 = jnp.bfloat16, jnp.float32
    hbm = pl.BlockSpec(memory_space=pltpu.HBM)
    anywhere = pl.BlockSpec(memory_space=pl.ANY)
    vmem = pl.BlockSpec(memory_space=pltpu.VMEM)
    local = (w_in.shape, w_in.shape, (model, cols), m_in.shape, m_in.shape)
    local += (w_out.shape, w_out.shape, (cols, model), m_in.shape, m_in.shape)
    outs = tuple(jax.ShapeDtypeStruct(shape, bf if n in (2, 7) else f32) for n, shape in enumerate(local))

    dma = pltpu.SemaphoreType.DMA
    results = pl.pallas_call(
        functools.partial(exchange, (F, T, Z, X, scale)),
        out_shape=outs,
        in_specs=[hbm] * 12,
        out_specs=(vmem,) * 10,
        scratch_shapes=[
            pltpu.VMEM((2, F, rows, rank), bf),
            pltpu.VMEM((F,) + w_in.shape, bf),
            pltpu.VMEM((F,) + w_out.shape, bf),
            pltpu.VMEM((F, 2, rr, cols), bf),
            pltpu.VMEM((cols, rank), bf),
            pltpu.VMEM((2, tokens, model), bf),
            pltpu.VMEM((2, tokens, cols), bf),
            pltpu.VMEM((2, rank, cols), f32),
            pltpu.VMEM((2, Z, X, rr, cols), bf),
            pltpu.VMEM((2, X, Z, rr, cols), bf),
            pltpu.VMEM((2, Z, rr, cols), bf),
            pltpu.VMEM((2, Z, rr, cols), bf),
            pltpu.VMEM((1, 128), f32),
            pltpu.VMEM((F * T, 1, 128), f32),
            pltpu.VMEM(w_in.shape, f32),
            pltpu.VMEM(w_out.shape, f32),
            *[pltpu.VMEM(m_in.shape, f32)] * 4,
            dma((2, chunks, 2)),
            dma((8,)),
            dma((4,)),
            dma((2, Z)),
            dma((2, Z, X - 1)),
            dma((2,)),
            dma((2,)),
            dma((2,)),
            dma((2, X - 1)),
            dma((2,)),
            dma((2,)),
            dma((2,)),
            dma((Z,)),
            dma((1,)),
            dma((3, WINDOW, X - 1)),
            dma((Z - 1, PIECES)),
            dma((Z - 1, PIECES)),
            dma((Z, PIECES, X - 1)),
        ],
        compiler_params=pltpu.CompilerParams(
            collective_id=0, has_side_effects=True, vmem_limit_bytes=VMEM_LIMIT
        ),
        name="exchange",
    )(
        *(
            pltpu.with_memory_space_constraint(array, pltpu.HBM)
            for array in (h, cc, oc, lo, basis_in, basis_out, w_in, w_out, m_in, v_in, m_out, v_out)
        )
    )

    return pl.pallas_call(
        flush,
        out_shape=outs,
        in_specs=[anywhere] * 10,
        out_specs=(anywhere,) * 10,
        scratch_shapes=[pltpu.SemaphoreType.DMA((10,))],
        compiler_params=pltpu.CompilerParams(vmem_limit_bytes=FLUSH_LIMIT),
        name="flush",
    )(*results)


def solution(mesh):
    split, both = P("fs", None), P("fs", "tp")
    return jax.shard_map(
        functools.partial(shards, mesh),
        mesh=mesh,
        in_specs=(split, both, both, split, split, split, both, P("tp", "fs"), both, both, both, both),
        out_specs=(both, both, P(None, "tp"), both, both, P("tp", "fs"), P("tp", "fs"), P("tp", None), both, both),
        check_vma=False,
    )
```

```python
import functools
import math

import jax
import jax.numpy as jnp
from jax import lax
from jax.experimental import pallas as pl
from jax.experimental.pallas import tpu as pltpu
from jax.sharding import PartitionSpec as P

MESH = pl.DeviceIdType.MESH
VMEM_LIMIT = 42 * 1024 * 1024
FLUSH_LIMIT = 1024 * 1024
PIECES = 8
DOUBLED = 2
WINDOW = 3
AHEAD = 6
PLAN = [(3, 3), (3, 3), (3, 3), [(1, 1)] * 4, [(1, 1), (0, 0)] * 2, (2, 1), (3, 2), (4, 3), (6, 5), (8, 6)]


def nt_dot(left, right):
    return lax.dot_general(left, right, (((1,), (1,)), ((), ())), preferred_element_type=jnp.float32)


def exchange(
    dims,
    h_hbm,
    cc_hbm,
    oc_hbm,
    lo_hbm,
    basis_in,
    basis_out,
    w_in_hbm,
    w_out_hbm,
    m_in_hbm,
    v_in_hbm,
    m_out_hbm,
    v_out_hbm,
    step_in,
    new_in,
    copy_in,
    nm_in,
    nv_in,
    step_out,
    new_out,
    copy_out,
    nm_out,
    nv_out,
    ball,
    win_all,
    wout_all,
    dall,
    turned,
    h_buf,
    c_buf,
    acc,
    part,
    x_part,
    z_sum,
    z_part,
    tot,
    tot_in,
    w_in,
    w_out,
    m_in,
    v_in,
    m_out,
    v_out,
    in_sem,
    load_sem,
    b_s,
    bz_r,
    bx_r,
    by_r,
    bm_r,
    p_s,
    px_r,
    pz_r,
    tot_sem,
    d_s,
    dz_r,
    dx_r,
    w_s,
    wd_r,
    wu_r,
    wx_r,
):
    F, T, Z, X, scale = dims
    Y, Q, D = T // 2, PIECES, DOUBLED
    R = Q + D * (X - 1)
    f = lax.axis_index("fs")
    t = lax.axis_index("tp")
    z, x = f // X, f % X
    y, core = t // 2, t % 2
    mate = t + 1 - 2 * core
    turn = 1 - 2 * ((2 * z) // Z)
    chunks = in_sem.shape[1]
    chunk = h_buf.shape[1] // chunks
    rr, cols = m_in.shape
    rows, rank = ball.shape[2:]
    quarter = rows // T

    def remote(src, dst, send, recv, device):
        return pltpu.make_async_remote_copy(
            src_ref=src, dst_ref=dst, send_sem=send, recv_sem=recv, device_id=device, device_id_type=MESH
        )

    def settle(ref, sem):
        pltpu.make_async_copy(ref, ref, sem).wait()

    def z_peer(k):
        return ((z + k) % Z) * X + x

    def x_peer(j):
        return z * X + (x + j) % X

    def fetch(which, i):
        span = pl.ds(i * chunk, chunk)
        h_src, c_src = ((h_hbm, cc_hbm), (oc_hbm, lo_hbm))[which]
        return (
            pltpu.make_async_copy(h_src.at[span], h_buf.at[which, span], in_sem.at[which, i, 0]),
            pltpu.make_async_copy(c_src.at[span], c_buf.at[which, span], in_sem.at[which, i, 1]),
        )

    barrier = pltpu.get_barrier_semaphore()

    def greet(device):
        pl.semaphore_signal(barrier, inc=1, device_id=device, device_id_type=MESH)

    for k in range(1, Z):
        greet((z_peer(k), t))
    for j in range(1, X):
        greet((x_peer(j), t))
    for i in range(1, Y):
        greet((f, ((y + i) % Y) * 2 + core))
    greet((f, mate))
    loads = [
        pltpu.make_async_copy(src, dst, load_sem.at[n])
        for n, (src, dst) in enumerate(
            (
                (basis_in, ball.at[0, f]),
                (basis_out, ball.at[1, f]),
                (w_in_hbm, w_in),
                (w_out_hbm, w_out),
                (m_in_hbm, m_in),
                (v_in_hbm, v_in),
                (m_out_hbm, m_out),
                (v_out_hbm, v_out),
            )
        )
    ]
    for copy in loads:
        copy.start()
    for which in range(2):
        for i in range(chunks):
            for copy in fetch(which, i):
                copy.start()
    own = pl.ds(pl.multiple_of(t * quarter, quarter), quarter)
    for copy in loads:
        copy.wait()
    win_all[f] = w_in[...].astype(jnp.bfloat16)
    wout_all[f] = w_out[...].astype(jnp.bfloat16)
    pl.semaphore_wait(barrier, (Z - 1) + (X - 1) + (Y - 1) + 1)

    def row(m):
        return (z + turn * m + Z) % Z

    def basis_at(which, m, j, part_of):
        s = row(m) * X + (x + X - j) % X
        return ball.at[which, s, pl.ds(pl.multiple_of(part_of * quarter, quarter), quarter)]

    def basis_z(which, k):
        at = ball.at[which, f, own]
        return remote(at, at, b_s.at[0], bz_r.at[which, z], (z_peer(k), t))

    def basis_z_arrival(which, m):
        at = basis_at(which, m, 0, t)
        return remote(at, at, b_s.at[0], bz_r.at[which, row(m)], (z_peer(1), t))

    def basis_x(which, m, j):
        at = basis_at(which, m, 0, t)
        return remote(at, at, b_s.at[1], bx_r.at[which, m, j - 1], (x_peer(j), t))

    def basis_x_arrival(which, m, j):
        at = basis_at(which, m, j, t)
        return remote(at, at, b_s.at[1], bx_r.at[which, m, j - 1], (x_peer(j), t))

    def basis_y(which, m, j, i):
        at = basis_at(which, m, j, t)
        return remote(at, at, b_s.at[2], by_r.at[which], (f, ((y + i) % Y) * 2 + core))

    def basis_mate(which, m, j, i):
        at = basis_at(which, m, j, ((y + Y - i) % Y) * 2 + core)
        return remote(at, at, b_s.at[3], bm_r.at[which], (f, mate))

    def basis_begin(which):
        for k in range(1, Z):
            basis_z(which, k).start()
        for j in range(1, X):
            basis_x(which, 0, j).start()

    def basis_spread(which, m, j):
        for i in range(1, Y):
            basis_y(which, m, j, i).start()
        basis_mate(which, m, j, 0).start()

    def basis_over_z(which):
        for m in range(1, Z):
            basis_z_arrival(which, m).wait_recv()
            for j in range(1, X):
                basis_x(which, m, j).start()
            basis_spread(which, m, 0)

    def basis_over_x(which):
        for m in range(Z):
            for j in range(1, X):
                basis_x_arrival(which, m, j).wait_recv()
                basis_spread(which, m, j)

    foreign = [(m, j) for j in range(X) for m in range(Z) if m or j]

    def basis_bytes(whiches, shares):
        return ball.at[whiches, pl.ds(0, F - 1), pl.ds(0, shares * quarter)]

    def basis_over_y(which):
        if Y > 1:
            settle(basis_bytes(which, Y - 1), by_r.at[which])
        for m, j in foreign:
            for i in range(1, Y):
                basis_mate(which, m, j, i).start()

    def basis_done(which):
        settle(basis_bytes(which, Y), bm_r.at[which])

    in_rows, out_rows = 2 * w_in.shape[0] // Q, 2 * w_out.shape[0] // Q

    def place(item, s, q):
        if item == 0:
            return win_all.at[s, pl.ds(pl.multiple_of((q // 2) * in_rows, in_rows), in_rows)]
        return wout_all.at[s, pl.ds(pl.multiple_of((q // 2) * out_rows, out_rows), out_rows)]

    def turns(q, body):
        for item in range(2):

            @pl.when(q % 2 == item)
            def _(item=item):
                body(item)

    def z_piece(n):
        m, r = n // R, n % R
        extra = r // Q
        j = extra * (1 + r // D - Q // D)
        return m, (x + X - j) % X, (1 - extra) * r + extra * (Q - D + r % D)

    def down(n, item):
        m, c, q = z_piece(n)
        at = place(item, (z + m) * X + c, q)
        return remote(at, at, w_s.at[0, n % WINDOW, 0], wd_r.at[n], ((z - 1) * X + x, t))

    def up(n, item):
        m, c, q = z_piece(n)
        at = place(item, (z - m) * X + c, q)
        return remote(at, at, w_s.at[1, n % WINDOW, 0], wu_r.at[n], ((z + 1) * X + x, t))

    def aside(n, m, q, item, j):
        at = place(item, row(m) * X + x, q)
        return remote(at, at, w_s.at[2, n % WINDOW, j - 1], wx_r.at[n, j - 1], (x_peer(j), t))

    def aside_arrival(n, m, q, item, j):
        at = place(item, row(m) * X + (x + X - j) % X, q)
        return remote(at, at, w_s.at[2, 0, j - 1], wx_r.at[n, j - 1], (x_peer(1), t))

    def down_arrival(n, item):
        m, c, q = z_piece(n)
        at = place(item, (z + m) * X + c, q)
        return remote(at, at, w_s.at[0, 0, 0], wd_r.at[n - R], (z_peer(1), t))

    def up_arrival(n, item):
        m, c, q = z_piece(n)
        at = place(item, (z - m) * X + c, q)
        return remote(at, at, w_s.at[1, 0, 0], wu_r.at[n - R], (z_peer(1), t))

    def goes_down(m):
        return (z >= 1) & (z + m <= Z - 1)

    def goes_up(m):
        return (z <= Z - 2) & (z - m >= 0)

    def z_settle(n):
        m = n // R

        @pl.when((n >= 0) & goes_down(m))
        def _():
            turns(n % R, lambda item: down(n, item).wait_send())

        @pl.when((n >= 0) & goes_up(m))
        def _():
            turns(n % R, lambda item: up(n, item).wait_send())

    def z_arrivals(n):
        m = n // R

        @pl.when((m >= 1) & (m <= Z - 1) & (z + m <= Z - 1))
        def _():
            turns(n % R, lambda item: down_arrival(n, item).wait_recv())

        @pl.when((m >= 1) & (m <= Z - 1) & (z - m >= 0))
        def _():
            turns(n % R, lambda item: up_arrival(n, item).wait_recv())

    def z_tick(n):
        m, r = n // R, n % R
        z_arrivals(n + AHEAD)
        z_settle(n - WINDOW)

        @pl.when((m == 0) & (r >= Q))
        def _():
            e = r % D
            turns(e, lambda item: aside_arrival(e, 0, Q - D + e, item, 1 + r // D - Q // D).wait_recv())

        @pl.when(goes_down(m))
        def _():
            turns(r, lambda item: down(n, item).start())

        @pl.when(goes_up(m))
        def _():
            turns(r, lambda item: up(n, item).start())

    def x_first(n):
        return 0, (n + Q - D) % Q

    def x_later(n):
        return 1 + (n - Q) // (Q - D), (n - Q) % (Q - D)

    def x_settle(n):
        for j in range(1, X):

            @pl.when((n >= 0) & (n < Q))
            def _(j=j):
                m, q = x_first(n)
                turns(q, lambda item: aside(n, m, q, item, j).wait_send())

            @pl.when(n >= Q)
            def _(j=j):
                m, q = x_later(n)
                turns(q, lambda item: aside(n, m, q, item, j).wait_send())

    def x_start(n, m, q):
        x_settle(n - WINDOW)
        for j in range(1, X):
            turns(q, lambda item: aside(n, m, q, item, j).start())

    def x_tick(n):
        @pl.when(n < Q)
        def _():
            x_start(n, *x_first(n))

        @pl.when(n >= Q)
        def _():
            x_start(n, *x_later(n))

    z_ticks, x_ticks = Z * R, Q + (Z - 1) * (Q - D)
    passed = [0, 0]

    def loop(low, high, body):
        def step(n, carry):
            body(n)
            return carry

        if high > low:
            lax.fori_loop(low, high, step, 0)

    def pump(z_count, x_count):
        z_at, x_at = passed
        z_count, x_count = max(0, min(z_count, z_ticks - z_at)), max(0, min(x_count, x_ticks - x_at))
        lead = max(0, z_count - x_count)

        def ready(n):
            m, q = x_later(x_at + n)
            return x_at + n < Q or m * R + q < min(z_at + min(z_count, lead + n + 1) + AHEAD, z_ticks + R)

        x_count = next((n for n in range(x_count) if not ready(n)), x_count)
        both = min(z_count - lead, x_count)

        def pair(n):
            z_tick(z_at + lead + n)
            x_tick(x_at + n)

        loop(z_at, z_at + lead, z_tick)
        loop(0, both, pair)
        loop(z_at + lead + both, z_at + z_count, z_tick)
        loop(x_at + both, x_at + x_count, x_tick)
        passed[0], passed[1] = z_at + z_count, x_at + x_count

    def project(which, during):
        acc[which] = jnp.zeros(acc.shape[1:], jnp.float32)
        for i in range(chunks):
            for copy in fetch(which, i):
                copy.wait()
            span = pl.ds(i * chunk, chunk)
            whole = ball[which].reshape(h_buf.shape[2], -1)
            reduced = jnp.dot(h_buf[which, span], whole, preferred_element_type=jnp.float32)
            turned_bf = reduced.T.astype(jnp.bfloat16)
            acc[which] += jnp.dot(turned_bf, c_buf[which, span], preferred_element_type=jnp.float32)
            during(i)
        part[which] = acc[which].astype(jnp.bfloat16).reshape(part.shape[1:])

    def part_x(which, j):
        return remote(
            part.at[which, pl.ds(0, Z), (x + j) % X],
            x_part.at[which, j],
            p_s.at[0],
            px_r.at[which, j - 1],
            (x_peer(j), t),
        )

    def part_z(which, k):
        return remote(
            z_sum.at[which, (z + k) % Z], z_part.at[which, k], p_s.at[1], pz_r.at[which], (z_peer(k), t)
        )

    def row_sum(which, to):
        value = acc[which, pl.ds(pl.multiple_of((to * X + x) * rr, rr), rr)]
        for j in range(1, X):
            value = value + x_part[which, j, to].astype(jnp.float32)
        return value

    def reduce_x(which):
        for j in range(1, X):
            part_x(which, j).wait_recv()
        for to in range(Z):
            z_sum[which, to] = row_sum(which, to).astype(jnp.bfloat16)
        for k in range(1, Z):
            part_z(which, k).start()

    def reduce_z(which):
        value = row_sum(which, z)
        settle(z_part.at[which, pl.ds(1, Z - 1)], pz_r.at[which])
        for k in range(1, Z):
            value = value + z_part[which, k].astype(jnp.float32)
        return value

    def share(n):
        return remote(
            tot,
            tot_in.at[n],
            tot_sem.at[0],
            tot_sem.at[1],
            ((f + n // T) % F, (t + n % T) % T),
        )

    def dir_z(k):
        return remote(dall.at[f], dall.at[f], d_s.at[0], dz_r.at[z], (z_peer(k), t))

    def dir_z_arrival(m):
        at = dall.at[row(m) * X + x]
        return remote(at, at, d_s.at[0], dz_r.at[row(m)], (z_peer(1), t))

    def dir_x(m, j):
        at = dall.at[row(m) * X + x]
        return remote(at, at, d_s.at[1], dx_r.at[0], (x_peer(j), t))

    def late(m):
        def each(n):
            at = x_later(n) if m else x_first(n)
            for j in range(1, X):
                turns(at[1], lambda item: aside_arrival(n, *at, item, j).wait_recv())

        loop(D if m == 0 else Q + (m - 1) * (Q - D), Q + m * (Q - D), each)

    def apply_own():
        direction = dall[:, 0].reshape(rank, cols)
        other = dall[:, 1].reshape(rank, cols)
        turned[...] = other.astype(jnp.float32).T.astype(jnp.bfloat16)
        step = jnp.dot(ball[0, f], direction, preferred_element_type=jnp.float32)
        step_in[...] = step
        new_in[...] = w_in[...] - 0.02 * step
        step = nt_dot(turned[...], ball[1, f])
        step_out[...] = step
        new_out[...] = w_out[...] - 0.02 * step

    def apply_row(m):
        direction = dall[:, 0].reshape(rank, cols)
        for j in range(X):
            s = row(m) * X + j
            span = pl.ds(pl.multiple_of(s * rows, rows), rows)
            step = jnp.dot(ball[0, s], direction, preferred_element_type=jnp.float32)
            copy_in[span] = (win_all[s].astype(jnp.float32) - 0.02 * step).astype(jnp.bfloat16)
            step = nt_dot(turned[...], ball[1, s])
            copy_out[:, span] = (wout_all[s].astype(jnp.float32) - 0.02 * step).astype(jnp.bfloat16)

    for which in range(2):
        basis_begin(which)
    pump(*PLAN[0])
    basis_over_z(0)
    basis_over_z(1)
    pump(*PLAN[1])
    basis_over_x(0)
    basis_over_x(1)
    pump(*PLAN[2])
    basis_over_y(0)
    basis_done(0)
    project(0, lambda i: pump(*PLAN[3][i % 4]))
    for j in range(1, X):
        part_x(0, j).start()
    basis_over_y(1)
    basis_done(1)

    def meanwhile(i):
        if i == min(2, chunks - 1):
            reduce_x(0)
        pump(*PLAN[4][i % 4])

    project(1, meanwhile)
    for j in range(1, X):
        part_x(1, j).start()
    pump(*PLAN[5])
    reduce_x(1)
    pump(*PLAN[6])
    projs = [reduce_z(which) for which in range(2)]
    square = sum(jnp.sum(value * value, axis=(0, 1), keepdims=True) for value in projs)
    tot[...] = jnp.broadcast_to(square, tot.shape)
    tot_in[0] = tot[...]
    loop(1, F * T, lambda n: share(n).start())
    pump(*PLAN[7])
    for sem in range(2):
        settle(tot_in.at[pl.ds(1, F * T - 1)], tot_sem.at[sem])
    total = jnp.sum(jnp.sum(tot_in[...], axis=0), axis=0, keepdims=True)
    factor = (scale * lax.rsqrt(total + 1e-06))[0:1, 0:1]
    for which, (first, second, first_to, second_to) in enumerate(
        ((m_in, v_in, nm_in, nv_in), (m_out, v_out, nm_out, nv_out))
    ):
        scaled = factor * projs[which]
        first_new = 0.8 * first[...] + 0.2 * scaled
        second_new = 0.9 * second[...] + 0.1 * scaled * scaled
        first_to[...] = first_new
        second_to[...] = second_new
        dall[f, which] = (first_new / (jnp.sqrt(second_new) + 1e-08)).astype(jnp.bfloat16)
    for k in range(1, Z):
        dir_z(k).start()
    for j in range(1, X):
        dir_x(0, j).start()
    pump(*PLAN[8])
    for m in range(1, Z):
        dir_z_arrival(m).wait_recv()
        for j in range(1, X):
            dir_x(m, j).start()
    pump(*PLAN[9])
    settle(dall.at[pl.ds(0, Z * (X - 1))], dx_r.at[0])
    apply_own()
    for m in range(Z):
        z_left, x_left = min(z_ticks, (m + 1) * R) - passed[0], Q + m * (Q - D) - passed[1]
        pump(z_left, x_left)
        assert passed[1] >= Q + m * (Q - D)
        late(m)
        apply_row(m)

    loop(z_ticks - WINDOW, z_ticks, z_settle)
    loop(x_ticks - WINDOW, x_ticks, x_settle)
    both = pl.ds(0, 2)
    settle(ball.at[both, pl.ds(0, Z - 1), pl.ds(0, quarter)], b_s.at[0])
    settle(ball.at[both, pl.ds(0, Z * (X - 1)), pl.ds(0, quarter)], b_s.at[1])
    if Y > 1:
        settle(basis_bytes(both, Y - 1), b_s.at[2])
    settle(basis_bytes(both, Y), b_s.at[3])
    settle(part.at[both, pl.ds(0, Z), pl.ds(0, X - 1)], p_s.at[0])
    settle(z_sum.at[both, pl.ds(0, Z - 1)], p_s.at[1])
    settle(dall.at[pl.ds(0, Z - 1)], d_s.at[0])
    settle(dall.at[pl.ds(0, Z * (X - 1))], d_s.at[1])


def flush(*refs):
    sources, targets, sems = refs[:10], refs[10:20], refs[20]
    copies = [pltpu.make_async_copy(a, b, sems.at[i]) for i, (a, b) in enumerate(zip(sources, targets))]
    for copy in copies:
        copy.start()
    for copy in copies:
        copy.wait()


def shards(mesh, h, cc, lo, oc, basis_in, basis_out, w_in, w_out, m_in, v_in, m_out, v_out):
    F, T = mesh.shape["fs"], mesh.shape["tp"]
    Z = next(n for n in range(1, F + 1) if F % n == 0 and n * n >= F)
    X, Y = F // Z, T // 2
    tokens, model = h.shape
    cols = cc.shape[1]
    rows, rank = basis_in.shape
    rr = m_in.shape[0]
    scale = math.sqrt(2.0 * rank * cols * T)
    chunks = max(1, tokens // 512)
    bf, f32 = jnp.bfloat16, jnp.float32
    hbm = pl.BlockSpec(memory_space=pltpu.HBM)
    anywhere = pl.BlockSpec(memory_space=pl.ANY)
    vmem = pl.BlockSpec(memory_space=pltpu.VMEM)
    local = (w_in.shape, w_in.shape, (model, cols), m_in.shape, m_in.shape)
    local += (w_out.shape, w_out.shape, (cols, model), m_in.shape, m_in.shape)
    outs = tuple(jax.ShapeDtypeStruct(shape, bf if n in (2, 7) else f32) for n, shape in enumerate(local))

    dma = pltpu.SemaphoreType.DMA
    results = pl.pallas_call(
        functools.partial(exchange, (F, T, Z, X, scale)),
        out_shape=outs,
        in_specs=[hbm] * 12,
        out_specs=(vmem,) * 10,
        scratch_shapes=[
            pltpu.VMEM((2, F, rows, rank), bf),
            pltpu.VMEM((F,) + w_in.shape, bf),
            pltpu.VMEM((F,) + w_out.shape, bf),
            pltpu.VMEM((F, 2, rr, cols), bf),
            pltpu.VMEM((cols, rank), bf),
            pltpu.VMEM((2, tokens, model), bf),
            pltpu.VMEM((2, tokens, cols), bf),
            pltpu.VMEM((2, rank, cols), f32),
            pltpu.VMEM((2, Z, X, rr, cols), bf),
            pltpu.VMEM((2, X, Z, rr, cols), bf),
            pltpu.VMEM((2, Z, rr, cols), bf),
            pltpu.VMEM((2, Z, rr, cols), bf),
            pltpu.VMEM((1, 128), f32),
            pltpu.VMEM((F * T, 1, 128), f32),
            pltpu.VMEM(w_in.shape, f32),
            pltpu.VMEM(w_out.shape, f32),
            *[pltpu.VMEM(m_in.shape, f32)] * 4,
            dma((2, chunks, 2)),
            dma((8,)),
            dma((4,)),
            dma((2, Z)),
            dma((2, Z, X - 1)),
            dma((2,)),
            dma((2,)),
            dma((2,)),
            dma((2, X - 1)),
            dma((2,)),
            dma((2,)),
            dma((2,)),
            dma((Z,)),
            dma((1,)),
            dma((3, WINDOW, X - 1)),
            dma(((Z - 1) * (PIECES + DOUBLED * (X - 1)),)),
            dma(((Z - 1) * (PIECES + DOUBLED * (X - 1)),)),
            dma((PIECES + (Z - 1) * (PIECES - DOUBLED), X - 1)),
        ],
        compiler_params=pltpu.CompilerParams(
            collective_id=0, has_side_effects=True, vmem_limit_bytes=VMEM_LIMIT
        ),
        name="exchange",
    )(
        *(
            pltpu.with_memory_space_constraint(array, pltpu.HBM)
            for array in (h, cc, oc, lo, basis_in, basis_out, w_in, w_out, m_in, v_in, m_out, v_out)
        )
    )

    return pl.pallas_call(
        flush,
        out_shape=outs,
        in_specs=[anywhere] * 10,
        out_specs=(anywhere,) * 10,
        scratch_shapes=[pltpu.SemaphoreType.DMA((10,))],
        compiler_params=pltpu.CompilerParams(vmem_limit_bytes=FLUSH_LIMIT),
        name="flush",
    )(*results)


def solution(mesh):
    split, both = P("fs", None), P("fs", "tp")
    return jax.shard_map(
        functools.partial(shards, mesh),
        mesh=mesh,
        in_specs=(split, both, both, split, split, split, both, P("tp", "fs"), both, both, both, both),
        out_specs=(both, both, P(None, "tp"), both, both, P("tp", "fs"), P("tp", "fs"), P("tp", None), both, both),
        check_vma=False,
    )
```
